32 devices in a mesh: fs: 8 (over z, x), tp: 4 (over y, core).
Axes of the slice: x: 2, y: 2, z: 4, core: 2. Of those that a mesh axis runs over, the one named last changes fastest.
Arguments:
- mixer_input: bfloat16 [8192, 4096], P('fs'), may hold values from -6 to 6
- cell_output: bfloat16 [8192, 2048], P('fs'), may hold values from -6 to 6
- query_grad: bfloat16 [8192, 2048], P('fs', 'tp'), may hold values from -4 to 4
- value_grad: bfloat16 [8192, 2048], P('fs', 'tp'), may hold values from -4 to 4
- output_grad: bfloat16 [8192, 4096], P('fs', 'tp'), may hold values from -4 to 4
- query_weight: float32 [4096, 2048], P('fs', 'tp'), may hold values from -6 to 6
- value_weight: float32 [4096, 2048], P('fs', 'tp'), may hold values from -6 to 6
- output_weight: float32 [2048, 4096], P('fs', 'tp'), may hold values from -6 to 6
- query_basis: bfloat16 [4096, 128], P('fs'), may hold values from -0.09375 to 0.09375
- value_basis: bfloat16 [4096, 128], P('fs'), may hold values from -0.09375 to 0.09375
- output_basis: bfloat16 [2048, 128], P('fs'), may hold values from -0.125 to 0.125
- query_mean: float32 [128, 2048], P(None, 'tp'), may hold values from -6 to 6
- value_mean: float32 [128, 2048], P(None, 'tp'), may hold values from -6 to 6
- output_mean: float32 [128, 4096], P(None, 'tp'), may hold values from -6 to 6
- query_square: float32 [128, 2048], P(None, 'tp'), may hold values from 0.25 to 4
- value_square: float32 [128, 2048], P(None, 'tp'), may hold values from 0.25 to 4
- output_square: float32 [128, 4096], P(None, 'tp'), may hold values from 0.25 to 4
Outputs:
- query_step: float32 [4096, 2048], P('fs', 'tp')
- value_step: float32 [4096, 2048], P('fs', 'tp')
- output_step: float32 [2048, 4096], P('fs', 'tp')
- query_copy: bfloat16 [4096, 2048], P(None, 'tp')
- value_copy: bfloat16 [4096, 2048], P(None, 'tp')
- output_copy: bfloat16 [2048, 4096], P(None, 'tp')
- query_first: float32 [128, 2048], P(None, 'tp')
- value_first: float32 [128, 2048], P(None, 'tp')
- output_first: float32 [128, 4096], P(None, 'tp')
- query_second: float32 [128, 2048], P(None, 'tp')
- value_second: float32 [128, 2048], P(None, 'tp')
- output_second: float32 [128, 4096], P(None, 'tp')
The draws below stay inside these ranges and needn't reach their ends.
All inputs are finite; a program needn't handle non-finite values.
Results may differ from the reference program's by a relative error of at most 0.013.
Values may be sent and summed in bfloat16 or wider, within the bound.
A program may use at most 128 MiB of HBM per device.

```python
import math
import jax
import jax.numpy as jnp
from jax import lax

MODEL = 4096
CELL = 2048
RANK = 128
TOKENS = 8192


def input_rows(key):
    return jnp.clip(jax.random.normal(jax.random.fold_in(key, 101), (TOKENS, MODEL), jnp.float32), -6.0, 6.0)


def readout_rows(key):
    return jnp.clip(jax.random.normal(jax.random.fold_in(key, 102), (TOKENS, CELL), jnp.float32), -6.0, 6.0)


def coherent_grad(key, rows, salt, width):
    inner = rows.shape[1]
    noise = jnp.clip(jax.random.normal(jax.random.fold_in(key, salt), (TOKENS, width), jnp.float32), -6.0, 6.0) * (1.0 / math.sqrt(TOKENS))
    heading = jax.random.normal(jax.random.fold_in(key, salt + 1), (inner,), jnp.float32) * (1.0 / math.sqrt(inner))
    column = jnp.clip(jax.random.normal(jax.random.fold_in(key, salt + 2), (width,), jnp.float32), -3.0, 3.0)
    strength = 4.0 * math.sqrt(inner) / TOKENS
    along = jnp.dot(rows, heading, precision=lax.Precision.HIGHEST)
    return jnp.clip(noise + strength * along[:, None] * column[None, :], -4.0, 4.0)


def draw_mixer_input(key, part):
    return input_rows(key).astype(jnp.bfloat16)


def draw_cell_output(key, part):
    return readout_rows(key).astype(jnp.bfloat16)


def draw_query_grad(key, part):
    return coherent_grad(key, input_rows(key), 201, CELL).astype(jnp.bfloat16)


def draw_value_grad(key, part):
    return coherent_grad(key, input_rows(key), 211, CELL).astype(jnp.bfloat16)


def draw_output_grad(key, part):
    return coherent_grad(key, readout_rows(key), 221, MODEL).astype(jnp.bfloat16)


def shard_levels(key, dims, pieces, low, high):
    level, own = 1.0, jax.random.fold_in(key, 6)
    for axis_at, blocks in pieces:
        heights = jnp.exp(jax.random.uniform(jax.random.fold_in(own, axis_at), (blocks,), jnp.float32, low / len(pieces), high / len(pieces)))
        level = level * jnp.repeat(heights, dims[axis_at] // blocks).reshape([-1 if axis == axis_at else 1 for axis in range(len(dims))])
    return level


def gaussian(own_key, extent, deviation, reach, cuts=(), kind=jnp.bfloat16):
    array = deviation * jax.random.normal(own_key, extent, jnp.float32)
    if cuts:
        array = array * shard_levels(own_key, extent, cuts, -0.22, 0.18)
    return jnp.clip(array, -reach, reach).astype(kind)


def setup_inputs(seed: int = 0) -> dict:
    seeds = jax.random.split(jax.random.key(seed), 18)
    return {
        "mixer_input": draw_mixer_input(jax.random.fold_in(seeds[17], 71), 0),
        "cell_output": draw_cell_output(jax.random.fold_in(seeds[17], 71), 0),
        "query_grad": draw_query_grad(jax.random.fold_in(seeds[17], 71), 0),
        "value_grad": draw_value_grad(jax.random.fold_in(seeds[17], 71), 0),
        "output_grad": draw_output_grad(jax.random.fold_in(seeds[17], 71), 0),
        "query_weight": gaussian(seeds[5], (MODEL, CELL), 1.0, 6.0, ((0, 8), (1, 4)), jnp.float32),
        "value_weight": gaussian(seeds[6], (MODEL, CELL), 1.0, 6.0, ((0, 8), (1, 4)), jnp.float32),
        "output_weight": gaussian(seeds[7], (CELL, MODEL), 1.0, 6.0, ((0, 8), (1, 4)), jnp.float32),
        "query_basis": gaussian(seeds[8], (MODEL, RANK), MODEL ** -0.5, 0.09375, ((0, 8),)),
        "value_basis": gaussian(seeds[9], (MODEL, RANK), MODEL ** -0.5, 0.09375, ((0, 8),)),
        "output_basis": gaussian(seeds[10], (CELL, RANK), CELL ** -0.5, 0.125, ((0, 8),)),
        "query_mean": gaussian(seeds[11], (RANK, CELL), 1.0, 6.0, ((1, 4),), jnp.float32),
        "value_mean": gaussian(seeds[12], (RANK, CELL), 1.0, 6.0, ((1, 4),), jnp.float32),
        "output_mean": gaussian(seeds[13], (RANK, MODEL), 1.0, 6.0, ((1, 4),), jnp.float32),
        "query_square": jnp.clip(jnp.exp(math.log(4.0) - 2.7725887 * jax.random.uniform(seeds[14], (RANK, CELL), jnp.float32) ** shard_levels(seeds[14], (RANK, CELL), ((1, 4),), -0.2, 0.2)), 0.25, 4.0),
        "value_square": jnp.clip(jnp.exp(math.log(4.0) - 2.7725887 * jax.random.uniform(seeds[15], (RANK, CELL), jnp.float32) ** shard_levels(seeds[15], (RANK, CELL), ((1, 4),), -0.2, 0.2)), 0.25, 4.0),
        "output_square": jnp.clip(jnp.exp(math.log(4.0) - 2.7725887 * jax.random.uniform(seeds[16], (RANK, MODEL), jnp.float32) ** shard_levels(seeds[16], (RANK, MODEL), ((1, 4),), -0.2, 0.2)), 0.25, 4.0),
    }


beta_first = 0.8
beta_second = 0.9
floor_mean = 0.005
learn_rate = 0.05

def across(leading, trailing):
    return lax.dot_general(leading, trailing, (((0,), (0,)), ((), ())), preferred_element_type=jnp.float32)

def moments(gradient, basis, mean_old, square_old):
    factor_full = basis.astype(jnp.float32)
    projected = lax.dot_general(factor_full, gradient, (((0,), (0,)), ((), ())), precision=lax.Precision.HIGHEST, preferred_element_type=jnp.float32)
    moment_one = beta_first * mean_old + (1.0 - beta_first) * projected
    moment_two = beta_second * square_old + (1.0 - beta_second) * projected * projected
    direction = moment_one / jnp.sqrt(moment_two)
    lowrank = jnp.dot(factor_full, direction, precision=lax.Precision.HIGHEST, preferred_element_type=jnp.float32)
    return (lowrank, moment_one, moment_two)

def reference(mixer_input, cell_output, query_grad, value_grad, output_grad, query_weight, value_weight, output_weight, query_basis, value_basis, output_basis, query_mean, value_mean, output_mean, query_square, value_square, output_square):
    gradient_query = across(mixer_input, query_grad)
    gradient_value = across(mixer_input, value_grad)
    gradient_output = across(cell_output, output_grad)
    low_query, query_first, query_second = moments(gradient_query, query_basis, query_mean, query_square)
    low_value, value_first, value_second = moments(gradient_value, value_basis, value_mean, value_square)
    low_output, output_first, output_second = moments(gradient_output, output_basis, output_mean, output_square)
    squares = jnp.sum(low_query * low_query) + jnp.sum(low_value * low_value) + jnp.sum(low_output * low_output)
    factor = 1.0 / jnp.sqrt(squares / (3.0 * MODEL * CELL) + floor_mean)
    query_step = -factor * low_query
    value_step = -factor * low_value
    output_step = -factor * low_output
    query_copy = (query_weight + learn_rate * query_step).astype(jnp.bfloat16)
    value_copy = (value_weight + learn_rate * value_step).astype(jnp.bfloat16)
    output_copy = (output_weight + learn_rate * output_step).astype(jnp.bfloat16)
    return (query_step, value_step, output_step, query_copy, value_copy, output_copy, query_first, value_first, output_first, query_second, value_second, output_second)
```

```python
import jax
import jax.numpy as jnp
from jax import lax
from jax.sharding import PartitionSpec as P

MODEL = 4096
CELL = 2048


beta_first = 0.8
beta_second = 0.9
floor_mean = 0.005
learn_rate = 0.05


def matmul(left, right):
    return jnp.dot(left, right, preferred_element_type=jnp.float32)


def split(value):
    high = lax.reduce_precision(value, 8, 7)
    return high.astype(jnp.bfloat16), (value - high).astype(jnp.bfloat16)


def send(value, target, count):
    return lax.ppermute(value, "fs", [(i, target(i)) for i in range(count)])


def routes(count, outer):
    inner = 2

    def cross(i):
        return i ^ 1

    def up(i):
        return (i // inner + 1) % outer * inner + i % inner

    def down(i):
        return (i // inner + outer - 1) % outer * inner + i % inner

    return cross, up, down


def first_hops(value, count):
    cross, up, down = routes(count, count // 2)
    return (
        send(value, cross, count),
        send(value, up, count),
        send(value, down, count),
    )


def gather(value, me, count, parity):
    if count != 8:
        return [(me, value)] + [
            ((me + count - k) % count, send(value, lambda i: (i + k) % count, count))
            for k in range(1, count)
        ]
    cross, up, down = routes(count, 4)
    beside, below, above = first_hops(value, count)
    beside_below = send(beside, up, count)
    beside_above = send(beside, down, count)
    far = send(below, up, count) if parity else send(above, down, count)
    far_beside = send(far, cross, count)
    return [
        (me, value),
        (cross(me), beside),
        (down(me), below),
        (up(me), above),
        (cross(down(me)), beside_below),
        (cross(up(me)), beside_above),
        (up(up(me)), far),
        (cross(up(up(me))), far_beside),
    ]


def assemble(pieces, count):
    rows = pieces[0][1].shape[0]
    whole = jnp.zeros((count * rows,) + pieces[0][1].shape[1:], pieces[0][1].dtype)
    for origin, piece in pieces:
        whole = lax.dynamic_update_slice(whole, piece, (origin * rows, 0))
    return whole


def sum_over_fs(part, me, count):
    rows = part.shape[0] // count

    def block(index):
        return lax.dynamic_slice(part, (index * rows, 0), (rows, part.shape[1]))

    total = block(me)
    for k in range(1, count):
        total = total + send(block((me + k) % count), lambda i: (i + k) % count, count)
    pieces = [(me, total)]
    for k in range(1, count):
        pieces.append(
            ((me + count - k) % count, send(total, lambda i: (i + k) % count, count))
        )
    return assemble(pieces, count)


def sum_over_tp(value, count):
    total = value
    for k in range(1, count):
        total = total + lax.ppermute(
            value, "tp", [(i, (i + k) % count) for i in range(count)]
        )
    return total


def moments(projected, mean_old, square_old):
    moment_one = beta_first * mean_old + (1.0 - beta_first) * projected
    moment_two = beta_second * square_old + (1.0 - beta_second) * projected * projected
    return (moment_one, moment_two, moment_one / jnp.sqrt(moment_two))


def gram(basis):
    return lax.dot_general(
        basis, basis, (((0,), (0,)), ((), ())), preferred_element_type=jnp.float32
    )


def norm(basis_gram, direction):
    return jnp.sum(
        direction * jnp.dot(basis_gram, direction, precision=lax.Precision.HIGHEST)
    )


def project(rows, grad):
    high, low = split(rows)
    both = lax.dot_general(
        jnp.concatenate([high, low], axis=1),
        grad,
        (((0,), (0,)), ((), ())),
        preferred_element_type=jnp.float32,
    )
    rank = rows.shape[1]
    return both[:rank] + both[rank:]


def twice(basis):
    return jnp.concatenate([basis, basis], axis=1)


def body(fs, tp):
    def local(
        mixer_input,
        cell_output,
        query_grad,
        value_grad,
        output_grad,
        query_weight,
        value_weight,
        output_weight,
        query_basis,
        value_basis,
        output_basis,
        query_mean,
        value_mean,
        output_mean,
        query_square,
        value_square,
        output_square,
    ):
        me = lax.axis_index("fs")
        rank = query_basis.shape[1]
        pair = jnp.concatenate([query_basis, value_basis], axis=1)
        whole_pair = assemble(gather(pair, me, fs, 0), fs)
        whole_output = assemble(gather(output_basis, me, fs, 1), fs)
        weights = [
            assemble(gather(weight.astype(jnp.bfloat16), me, fs, parity), fs)
            for weight, parity in ((query_weight, 0), (value_weight, 1), (output_weight, 0))
        ]
        rows_pair = matmul(mixer_input, whole_pair)
        rows_output = matmul(cell_output, whole_output)
        part = jnp.concatenate(
            [
                project(rows_pair[:, :rank], query_grad),
                project(rows_pair[:, rank:], value_grad),
                project(rows_output, output_grad),
            ],
            axis=1,
        )
        projected = sum_over_fs(part, me, fs)
        width = query_grad.shape[1]
        proj = (
            projected[:, :width],
            projected[:, width : 2 * width],
            projected[:, 2 * width :],
        )
        means = (query_mean, value_mean, output_mean)
        olds = (query_square, value_square, output_square)
        firsts, seconds, dirs = zip(*(moments(*each) for each in zip(proj, means, olds)))
        bases = (whole_pair[:, :rank], whole_pair[:, rank:], whole_output)
        partial_squares = sum(norm(gram(b), d) for b, d in zip(bases, dirs))
        squares = sum_over_tp(jnp.full((8, 128), partial_squares, jnp.float32), tp)[0, 0]
        factor = 1.0 / jnp.sqrt(squares / (3.0 * MODEL * CELL) + floor_mean)
        pairs = [jnp.concatenate(split(d), axis=0) for d in dirs]
        steps = [
            -factor * matmul(twice(b), d)
            for b, d in zip((query_basis, value_basis, output_basis), pairs)
        ]
        copies = [
            (w.astype(jnp.float32) + (-learn_rate * factor) * matmul(twice(b), d)).astype(
                jnp.bfloat16
            )
            for w, b, d in zip(weights, bases, pairs)
        ]
        return (*steps, *copies, *firsts, *seconds)

    return local


def solution(mesh):
    rows, split_both, columns = P("fs", None), P("fs", "tp"), P(None, "tp")
    in_specs = (rows,) * 2 + (split_both,) * 6 + (rows,) * 3 + (columns,) * 6
    out_specs = (split_both,) * 3 + (columns,) * 9
    return jax.shard_map(
        body(mesh.shape["fs"], mesh.shape["tp"]),
        mesh=mesh,
        in_specs=in_specs,
        out_specs=out_specs,
        check_vma=False,
    )
```

```python
import functools

import jax
import jax.numpy as jnp
from jax import lax
from jax.experimental import pallas as pl
from jax.experimental.pallas import tpu as pltpu
from jax.sharding import PartitionSpec as P

MODEL = 4096
CELL = 2048


beta_first = 0.8
beta_second = 0.9
floor_mean = 0.005
learn_rate = 0.05

MESH = pl.DeviceIdType.MESH


def matmul(left, right):
    return jnp.dot(left, right, preferred_element_type=jnp.float32)


def split(value):
    high = lax.reduce_precision(value, 8, 7)
    return high.astype(jnp.bfloat16), (value - high).astype(jnp.bfloat16)


def moments(projected, mean_old, square_old):
    moment_one = beta_first * mean_old + (1.0 - beta_first) * projected
    moment_two = beta_second * square_old + (1.0 - beta_second) * projected * projected
    return (moment_one, moment_two, moment_one / jnp.sqrt(moment_two))


def twice(basis):
    return jnp.concatenate([basis, basis], axis=1)


class Gather:
    def __init__(self, number, own, whole, me, count, parity, send_sem, recv_sem):
        self.number, self.own, self.whole, self.me = number, own, whole, me
        self.count, self.parity = count, parity
        self.send_sem, self.recv_sem = send_sem, recv_sem
        self.rows = whole.shape[0] // count
        self.sent = []
        self.relayed = count == 8
        place, side = me // 2, lax.rem(me, 2)
        self.cross = place * 2 + (1 - side)
        self.up = lax.rem(place + 1, 4) * 2 + side
        self.down = lax.rem(place + 3, 4) * 2 + side
        up_cross = lax.rem(place + 1, 4) * 2 + (1 - side)
        down_cross = lax.rem(place + 3, 4) * 2 + (1 - side)
        far = lax.rem(place + 2, 4) * 2 + side
        far_cross = lax.rem(place + 2, 4) * 2 + (1 - side)
        if self.relayed:
            self.origins = [
                self.cross, self.down, self.up, down_cross, up_cross, far, far_cross
            ]
        else:
            self.origins = [lax.rem(me + count - k, count) for k in range(1, count)]

    def slot(self, origin):
        return self.whole.at[pl.ds(pl.multiple_of(origin * self.rows, self.rows), self.rows), :]

    def copy(self, role, source, origin, target):
        return pltpu.make_async_remote_copy(
            src_ref=source,
            dst_ref=self.slot(origin),
            send_sem=self.send_sem.at[self.number, role],
            recv_sem=self.recv_sem.at[self.number, role],
            device_id={"fs": target},
            device_id_type=MESH,
        )

    def send(self, role, origin, target, source=None):
        copy = self.copy(role, self.slot(origin) if source is None else source, origin, target)
        copy.start()
        self.sent.append(copy)

    def arrive(self, role):
        origin = self.origins[role]
        self.copy(role, self.slot(origin), origin, self.cross).wait_recv()

    def start(self):
        if self.relayed:
            for role, target in enumerate((self.cross, self.up, self.down)):
                self.send(role, self.me, target, self.own)
        else:
            for k in range(1, self.count):
                self.send(k - 1, self.me, lax.rem(self.me + k, self.count), self.own)

    def middle(self):
        if self.relayed:
            self.arrive(0)
            self.send(3, self.origins[0], self.up)
            self.send(4, self.origins[0], self.down)
            self.arrive(1)
            if self.parity:
                self.send(5, self.origins[1], self.up)
            self.arrive(2)
            if not self.parity:
                self.send(5, self.origins[2], self.down)

    def late(self):
        if self.relayed:
            self.arrive(5)
            self.send(6, self.origins[5], self.cross)

    def finish(self):
        for role in (3, 4, 6) if self.relayed else range(self.count - 1):
            self.arrive(role)

    def drain(self):
        for copy in self.sent:
            copy.wait_send()


def kernel(
    fs,
    tp,
    mixer_hbm,
    cell_hbm,
    qg_hbm,
    vg_hbm,
    og_hbm,
    pair_hbm,
    ob_hbm,
    qw_hbm,
    vw_hbm,
    ow_hbm,
    qm,
    vm,
    om,
    qs,
    vs,
    os,
    qw_all,
    vw_all,
    ow_all,
    pair_all,
    ob_all,
    proj,
    squares,
    mixer,
    cell,
    qg,
    vg,
    og,
    qw,
    vw,
    ow,
    part,
    parts,
    square_own,
    square_in,
    send_sem,
    recv_sem,
    sum_send,
    sum_recv,
    all_send,
    all_recv,
    tp_send,
    tp_recv,
    local_sem,
):
    me, column = lax.axis_index("fs"), lax.axis_index("tp")
    rank, width = qm.shape
    gathers = [
        Gather(i, own, whole, me, fs, parity, send_sem, recv_sem)
        for i, (own, whole, parity) in enumerate(
            ((None, pair_all, 0), (None, ob_all, 1), (qw, qw_all, 0), (vw, vw_all, 1), (ow, ow_all, 0))
        )
    ]
    for gather in gathers[:2]:
        gather.own = gather.slot(me)
    loads = [
        pltpu.make_async_copy(source, target, local_sem.at[i])
        for i, (source, target) in enumerate(
            (
                (pair_hbm, gathers[0].own),
                (ob_hbm, gathers[1].own),
                (qw_hbm, qw),
                (vw_hbm, vw),
                (ow_hbm, ow),
                (cell_hbm, cell),
                (og_hbm, og),
                (mixer_hbm, mixer),
                (qg_hbm, qg),
                (vg_hbm, vg),
            )
        )
    ]
    for load in loads:
        load.start()

    barrier = pltpu.get_barrier_semaphore()
    for k in range(1, fs):
        pl.semaphore_signal(
            barrier, inc=1, device_id={"fs": lax.rem(me + k, fs)}, device_id_type=MESH
        )
    for k in range(1, tp):
        pl.semaphore_signal(
            barrier, inc=1, device_id={"tp": lax.rem(column + k, tp)}, device_id_type=MESH
        )
    pl.semaphore_wait(barrier, fs + tp - 2)

    pair_g, ob_g, qw_g, vw_g, ow_g = gathers
    loads[0].wait()
    pair_g.start()
    loads[1].wait()
    ob_g.start()
    loads[2].wait()
    qw_g.start()
    pair_g.middle()
    ob_g.middle()
    pair_g.late()
    ob_g.late()
    loads[3].wait()
    vw_g.start()
    loads[4].wait()
    ow_g.start()
    keeps = [
        pltpu.make_async_copy(gather.own, gather.slot(me), local_sem.at[10 + i])
        for i, gather in enumerate(gathers[2:])
    ]
    for keep in keeps:
        keep.start()
    qw_g.middle()
    for load in loads[5:]:
        load.wait()
    part[...] = jnp.zeros_like(part)
    pair_g.finish()
    ob_g.finish()

    tile = 256

    def project(rows, grad):
        turned = jnp.transpose(rows)
        high = turned.astype(jnp.bfloat16)
        low = (turned - high.astype(jnp.float32)).astype(jnp.bfloat16)
        both = matmul(jnp.concatenate([high, low], axis=0), grad)
        return both[:rank] + both[rank:]

    def step(t, carry):
        at = pl.ds(pl.multiple_of(t * tile, tile), tile)
        rows = matmul(mixer[at, :], pair_all[...])
        part[:, :width] += project(rows[:, :rank], qg[at, :])
        part[:, width : 2 * width] += project(rows[:, rank:], vg[at, :])
        part[:, 2 * width :] += project(matmul(cell[at, :], ob_all[...]), og[at, :])
        return carry

    lax.fori_loop(0, mixer.shape[0] // tile, step, 0)

    share = rank // fs

    def strip(index):
        return pl.ds(pl.multiple_of(index * share, share), share)

    sums = []
    for k in range(1, fs):
        target = lax.rem(me + k, fs)
        copy = pltpu.make_async_remote_copy(
            src_ref=part.at[strip(target), :],
            dst_ref=parts.at[k - 1],
            send_sem=sum_send.at[k - 1],
            recv_sem=sum_recv.at[k - 1],
            device_id={"fs": target},
            device_id_type=MESH,
        )
        copy.start()
        sums.append(copy)
    vw_g.middle()
    qw_g.late()

    def gram(whole, block):
        def add(i, total):
            piece = whole[pl.ds(pl.multiple_of(i * block, block), block), :]
            turned = jnp.transpose(piece.astype(jnp.float32)).astype(jnp.bfloat16)
            return total + matmul(turned, piece)

        size = whole.shape[1]
        return lax.fori_loop(
            0, whole.shape[0] // block, add, jnp.zeros((size, size), jnp.float32)
        )

    for copy in sums:
        copy.wait_recv()
    total = part[strip(me), :]
    for k in range(1, fs):
        total = total + parts[k - 1]
    proj[strip(me), :] = total
    gram_pair = gram(pair_all, 256)
    gram_output = gram(ob_all, 256)
    alls = []
    for k in range(1, fs):
        copy = pltpu.make_async_remote_copy(
            src_ref=proj.at[strip(me), :],
            dst_ref=proj.at[strip(me), :],
            send_sem=all_send.at[k - 1],
            recv_sem=all_recv.at[k - 1],
            device_id={"fs": lax.rem(me + k, fs)},
            device_id_type=MESH,
        )
        copy.start()
        alls.append(copy)
    ow_g.middle()
    vw_g.late()
    for k in range(1, fs):
        origin = lax.rem(me + fs - k, fs)
        pltpu.make_async_remote_copy(
            src_ref=proj.at[strip(origin), :],
            dst_ref=proj.at[strip(origin), :],
            send_sem=all_send.at[k - 1],
            recv_sem=all_recv.at[k - 1],
            device_id={"fs": lax.rem(me + k, fs)},
            device_id_type=MESH,
        ).wait_recv()

    def norm(basis_gram, projected, mean, square):
        direction = moments(projected, mean[...], square[...])[2]
        turned = jnp.dot(
            basis_gram,
            direction,
            precision=lax.Precision.HIGHEST,
            preferred_element_type=jnp.float32,
        )
        lanes = jnp.sum(direction * turned, axis=0, keepdims=True)
        return jnp.sum(lanes, axis=1, keepdims=True)

    partial = (
        norm(gram_pair[:rank, :rank], proj[:, :width], qm, qs)
        + norm(gram_pair[rank:, rank:], proj[:, width : 2 * width], vm, vs)
        + norm(gram_output, proj[:, 2 * width :], om, os)
    )
    square_own[...] = jnp.broadcast_to(partial, square_own.shape)
    ow_g.late()
    shares = []
    for k in range(1, tp):
        copy = pltpu.make_async_remote_copy(
            src_ref=square_own,
            dst_ref=square_in.at[k - 1],
            send_sem=tp_send.at[k - 1],
            recv_sem=tp_recv.at[k - 1],
            device_id={"tp": lax.rem(column + k, tp)},
            device_id_type=MESH,
        )
        copy.start()
        shares.append(copy)
    for copy in shares:
        copy.wait_recv()
    whole_squares = square_own[...]
    for k in range(1, tp):
        whole_squares = whole_squares + square_in[k - 1]
    squares[...] = whole_squares
    for gather in gathers[2:]:
        gather.finish()
    for copy in sums + alls + shares:
        copy.wait_send()
    for gather in gathers:
        gather.drain()
    for keep in keeps:
        keep.wait()


def exchange(fs, tp, mixer, cell, grads, pair, output_basis, weights, means, olds):
    share = pair.shape[1] // 2 // fs
    total = sum(grad.shape[1] for grad in grads)
    rank = means[0].shape[0]
    bf16, f32 = jnp.bfloat16, jnp.float32
    places = max(fs - 1, 7)
    hbm, vmem = pl.BlockSpec(memory_space=pl.ANY), pl.BlockSpec(memory_space=pltpu.VMEM)
    dma = pltpu.SemaphoreType.DMA

    def whole(array):
        return jax.ShapeDtypeStruct((array.shape[0] * fs, array.shape[1]), bf16)

    return pl.pallas_call(
        functools.partial(kernel, fs, tp),
        out_shape=(
            *(whole(weight) for weight in weights),
            whole(pair),
            whole(output_basis),
            jax.ShapeDtypeStruct((rank, total), f32),
            jax.ShapeDtypeStruct((8, 128), f32),
        ),
        in_specs=[hbm] * 10 + [vmem] * 6,
        out_specs=(hbm,) * 3 + (vmem,) * 4,
        scratch_shapes=[
            *(pltpu.VMEM(array.shape, bf16) for array in (mixer, cell, *grads, *weights)),
            pltpu.VMEM((rank, total), f32),
            pltpu.VMEM((fs - 1, share, total), f32),
            pltpu.VMEM((8, 128), f32),
            pltpu.VMEM((tp - 1, 8, 128), f32),
            dma((5, places)),
            dma((5, places)),
            dma((fs - 1,)),
            dma((fs - 1,)),
            dma((fs - 1,)),
            dma((fs - 1,)),
            dma((tp - 1,)),
            dma((tp - 1,)),
            dma((13,)),
        ],
        compiler_params=pltpu.CompilerParams(
            collective_id=0, has_side_effects=True, vmem_limit_bytes=50 * 1024 * 1024
        ),
    )(mixer, cell, *grads, pair, output_basis, *weights, *means, *olds)


def body(fs, tp):
    def local(
        mixer_input,
        cell_output,
        query_grad,
        value_grad,
        output_grad,
        query_weight,
        value_weight,
        output_weight,
        query_basis,
        value_basis,
        output_basis,
        query_mean,
        value_mean,
        output_mean,
        query_square,
        value_square,
        output_square,
    ):
        rank = query_basis.shape[1]
        means = (query_mean, value_mean, output_mean)
        olds = (query_square, value_square, output_square)
        *weights, whole_pair, whole_output, projected, squares = exchange(
            fs,
            tp,
            mixer_input,
            cell_output,
            (query_grad, value_grad, output_grad),
            jnp.concatenate([query_basis, value_basis], axis=1),
            output_basis,
            [w.astype(jnp.bfloat16) for w in (query_weight, value_weight, output_weight)],
            means,
            olds,
        )
        width = query_grad.shape[1]
        proj = (
            projected[:, :width],
            projected[:, width : 2 * width],
            projected[:, 2 * width :],
        )
        firsts, seconds, dirs = zip(*(moments(*each) for each in zip(proj, means, olds)))
        bases = (whole_pair[:, :rank], whole_pair[:, rank:], whole_output)
        factor = 1.0 / jnp.sqrt(squares[0, 0] / (3.0 * MODEL * CELL) + floor_mean)
        pairs = [jnp.concatenate(split(d), axis=0) for d in dirs]
        steps = [
            -factor * matmul(twice(b), d)
            for b, d in zip((query_basis, value_basis, output_basis), pairs)
        ]
        copies = [
            (w.astype(jnp.float32) + (-learn_rate * factor) * matmul(twice(b), d)).astype(
                jnp.bfloat16
            )
            for w, b, d in zip(weights, bases, pairs)
        ]
        return (*steps, *copies, *firsts, *seconds)

    return local


def solution(mesh):
    rows, split_both, columns = P("fs", None), P("fs", "tp"), P(None, "tp")
    in_specs = (rows,) * 2 + (split_both,) * 6 + (rows,) * 3 + (columns,) * 6
    out_specs = (split_both,) * 3 + (columns,) * 9
    return jax.shard_map(
        body(mesh.shape["fs"], mesh.shape["tp"]),
        mesh=mesh,
        in_specs=in_specs,
        out_specs=out_specs,
        check_vma=False,
    )
```

```python
import functools

import jax
import jax.numpy as jnp
from jax import lax
from jax.experimental import pallas as pl
from jax.experimental.pallas import tpu as pltpu
from jax.sharding import PartitionSpec as P

MODEL = 4096
CELL = 2048


beta_first = 0.8
beta_second = 0.9
floor_mean = 0.005
learn_rate = 0.05

MESH = pl.DeviceIdType.MESH


def matmul(left, right):
    return jnp.dot(left, right, preferred_element_type=jnp.float32)


def split(value):
    high = lax.reduce_precision(value, 8, 7)
    return high.astype(jnp.bfloat16), (value - high).astype(jnp.bfloat16)


def moments(projected, mean_old, square_old):
    moment_one = beta_first * mean_old + (1.0 - beta_first) * projected
    moment_two = beta_second * square_old + (1.0 - beta_second) * projected * projected
    return (moment_one, moment_two, moment_one / jnp.sqrt(moment_two))


def twice(basis):
    return jnp.concatenate([basis, basis], axis=1)


class Gather:
    def __init__(self, number, own, whole, block, half, me, count, by_line, send_sem, recv_sem):
        self.number, self.whole, self.block, self.half = number, whole, block, half
        self.me, self.count, self.by_line = me, count, by_line
        self.send_sem, self.recv_sem = send_sem, recv_sem
        self.rows = block // 2 if half is not None else block
        self.sent = []
        self.relayed = count == 8
        self.place, self.side = me // 2, lax.rem(me, 2)
        self.own = self.slot(me) if own is None else own

    def index(self, step, other=False):
        place = lax.rem(self.place + step + 4, 4)
        return place * 2 + (1 - self.side if other else self.side)

    def slot(self, origin):
        start = pl.multiple_of(origin * self.block, self.block)
        if self.half:
            start = pl.multiple_of(start + self.rows, self.rows)
        return self.whole.at[pl.ds(start, self.rows), :]

    def send(self, role, origin, target, inside=None, source=None):
        copy = pltpu.make_async_remote_copy(
            src_ref=self.slot(origin) if source is None else source,
            dst_ref=self.slot(origin),
            send_sem=self.send_sem.at[self.number, len(self.sent)],
            recv_sem=self.recv_sem.at[self.number, role],
            device_id={"fs": target},
            device_id_type=MESH,
        )
        self.sent.append((copy, inside))
        if inside is None:
            copy.start()
        else:
            pl.when(inside)(copy.start)

    def arrive(self, role, origin, inside=None):
        copy = pltpu.make_async_remote_copy(
            src_ref=self.slot(origin),
            dst_ref=self.slot(origin),
            send_sem=self.send_sem.at[self.number, 0],
            recv_sem=self.recv_sem.at[self.number, role],
            device_id={"fs": lax.rem(self.me + 1, self.count)},
            device_id_type=MESH,
        )
        if inside is None:
            copy.wait_recv()
        else:
            pl.when(inside)(copy.wait_recv)

    def start(self):
        if self.relayed:
            self.send(0, self.me, self.index(1), self.place < 3, self.own)
            self.send(3, self.me, self.index(-1), self.place > 0, self.own)
            self.send(6, self.me, self.index(0, True), None, self.own)
        else:
            for k in range(1, self.count):
                self.send(k - 1, self.me, lax.rem(self.me + k, self.count), None, self.own)

    def relay(self, distance):
        if not self.relayed:
            return
        place = self.place
        across = not (self.by_line and distance == 1)
        cross = self.index(0, True)
        if not across:
            self.arrive(6, cross)
            self.send(7, cross, self.index(1), place < 3)
            self.send(10, cross, self.index(-1), place > 0)
        below, above = self.index(-distance), self.index(distance)
        from_below, from_above = place >= distance, place + distance < 4
        self.arrive(distance - 1, below, from_below)
        if distance < 3:
            self.send(distance, below, self.index(1), (place >= distance) & (place < 3))
        if across:
            self.send(6 + distance, below, cross, from_below)
        self.arrive(2 + distance, above, from_above)
        if distance < 3:
            self.send(3 + distance, above, self.index(-1), from_above & (place > 0))
        if across:
            self.send(9 + distance, above, cross, from_above)

    def finish(self):
        if not self.relayed:
            for k in range(1, self.count):
                self.arrive(k - 1, lax.rem(self.me + self.count - k, self.count))
            return
        if not self.by_line:
            self.arrive(6, self.index(0, True))
        for distance in range(1, 4):
            self.arrive(6 + distance, self.index(-distance, True), self.place >= distance)
            self.arrive(9 + distance, self.index(distance, True), self.place + distance < 4)

    def drain(self):
        for copy, inside in self.sent:
            if inside is None:
                copy.wait_send()
            else:
                pl.when(inside)(copy.wait_send)


def kernel(
    fs,
    tp,
    mixer_hbm,
    cell_hbm,
    qg_hbm,
    vg_hbm,
    og_hbm,
    pair_hbm,
    ob_hbm,
    qw_hbm,
    vw_hbm,
    ow_hbm,
    qm,
    vm,
    om,
    qs,
    vs,
    os,
    qw_all,
    vw_all,
    ow_all,
    pair_all,
    ob_all,
    proj,
    squares,
    mixer,
    cell,
    qg,
    vg,
    og,
    qw,
    vw,
    ow,
    part,
    parts,
    square_own,
    square_in,
    send_sem,
    recv_sem,
    sum_send,
    sum_recv,
    all_send,
    all_recv,
    tp_send,
    tp_recv,
    local_sem,
):
    me, column = lax.axis_index("fs"), lax.axis_index("tp")
    rank, width = qm.shape
    gathers = [
        Gather(0, None, pair_all, pair_hbm.shape[0], None, me, fs, False, send_sem, recv_sem),
        Gather(1, None, ob_all, ob_hbm.shape[0], None, me, fs, True, send_sem, recv_sem),
    ]
    kept = ((qw, qw_all), (vw, vw_all), (ow, ow_all))
    for own, whole in kept:
        block = own.shape[0]
        for half in range(2):
            piece = own.at[pl.ds(half * (block // 2), block // 2), :]
            gathers.append(
                Gather(
                    len(gathers), piece, whole, block, half, me, fs, half == 0, send_sem, recv_sem
                )
            )
    loads = [
        pltpu.make_async_copy(source, target, local_sem.at[i])
        for i, (source, target) in enumerate(
            (
                (pair_hbm, gathers[0].own),
                (ob_hbm, gathers[1].own),
                (qw_hbm, qw),
                (vw_hbm, vw),
                (ow_hbm, ow),
                (cell_hbm, cell),
                (og_hbm, og),
                (mixer_hbm, mixer),
                (qg_hbm, qg),
                (vg_hbm, vg),
            )
        )
    ]
    for load in loads:
        load.start()

    barrier = pltpu.get_barrier_semaphore()
    for k in range(1, fs):
        pl.semaphore_signal(
            barrier, inc=1, device_id={"fs": lax.rem(me + k, fs)}, device_id_type=MESH
        )
    for k in range(1, tp):
        pl.semaphore_signal(
            barrier, inc=1, device_id={"tp": lax.rem(column + k, tp)}, device_id_type=MESH
        )
    pl.semaphore_wait(barrier, fs + tp - 2)

    loads[0].wait()
    gathers[0].start()
    loads[1].wait()
    gathers[1].start()
    loads[2].wait()
    gathers[2].start()
    for distance in range(1, 4):
        gathers[0].relay(distance)
        gathers[1].relay(distance)
    gathers[3].start()
    loads[3].wait()
    gathers[4].start()
    gathers[5].start()
    loads[4].wait()
    gathers[6].start()
    gathers[7].start()
    keeps = []
    for i, (own, whole) in enumerate(kept):
        rows = own.shape[0]
        place = whole.at[pl.ds(pl.multiple_of(me * rows, rows), rows), :]
        keeps.append(pltpu.make_async_copy(own, place, local_sem.at[10 + i]))
    for keep in keeps:
        keep.start()
    gathers[2].relay(1)
    for load in loads[5:]:
        load.wait()
    part[...] = jnp.zeros_like(part)
    gathers[0].finish()
    gathers[1].finish()

    tile = 256

    def project(rows, grad):
        turned = jnp.transpose(rows)
        high = turned.astype(jnp.bfloat16)
        low = (turned - high.astype(jnp.float32)).astype(jnp.bfloat16)
        both = matmul(jnp.concatenate([high, low], axis=0), grad)
        return both[:rank] + both[rank:]

    def step(t, carry):
        at = pl.ds(pl.multiple_of(t * tile, tile), tile)
        rows = matmul(mixer[at, :], pair_all[...])
        part[:, :width] += project(rows[:, :rank], qg[at, :])
        part[:, width : 2 * width] += project(rows[:, rank:], vg[at, :])
        part[:, 2 * width :] += project(matmul(cell[at, :], ob_all[...]), og[at, :])
        return carry

    lax.fori_loop(0, mixer.shape[0] // tile, step, 0)

    share = rank // fs

    def strip(index):
        return pl.ds(pl.multiple_of(index * share, share), share)

    sums = []
    for k in range(1, fs):
        target = lax.rem(me + k, fs)
        copy = pltpu.make_async_remote_copy(
            src_ref=part.at[strip(target), :],
            dst_ref=parts.at[k - 1],
            send_sem=sum_send.at[k - 1],
            recv_sem=sum_recv.at[k - 1],
            device_id={"fs": target},
            device_id_type=MESH,
        )
        copy.start()
        sums.append(copy)
    gathers[3].relay(1)
    gathers[2].relay(2)
    gathers[4].relay(1)
    gathers[3].relay(2)
    gathers[2].relay(3)

    def gram(whole, block):
        def add(i, total):
            piece = whole[pl.ds(pl.multiple_of(i * block, block), block), :]
            turned = jnp.transpose(piece.astype(jnp.float32)).astype(jnp.bfloat16)
            return total + matmul(turned, piece)

        size = whole.shape[1]
        return lax.fori_loop(
            0, whole.shape[0] // block, add, jnp.zeros((size, size), jnp.float32)
        )

    for copy in sums:
        copy.wait_recv()
    total = part[strip(me), :]
    for k in range(1, fs):
        total = total + parts[k - 1]
    proj[strip(me), :] = total
    gram_pair = gram(pair_all, 256)
    gram_output = gram(ob_all, 256)
    alls = []
    for k in range(1, fs):
        copy = pltpu.make_async_remote_copy(
            src_ref=proj.at[strip(me), :],
            dst_ref=proj.at[strip(me), :],
            send_sem=all_send.at[k - 1],
            recv_sem=all_recv.at[k - 1],
            device_id={"fs": lax.rem(me + k, fs)},
            device_id_type=MESH,
        )
        copy.start()
        alls.append(copy)
    gathers[5].relay(1)
    gathers[4].relay(2)
    gathers[3].relay(3)
    gathers[6].relay(1)
    gathers[5].relay(2)
    gathers[4].relay(3)
    gathers[7].relay(1)
    for k in range(1, fs):
        origin = lax.rem(me + fs - k, fs)
        pltpu.make_async_remote_copy(
            src_ref=proj.at[strip(origin), :],
            dst_ref=proj.at[strip(origin), :],
            send_sem=all_send.at[k - 1],
            recv_sem=all_recv.at[k - 1],
            device_id={"fs": lax.rem(me + k, fs)},
            device_id_type=MESH,
        ).wait_recv()

    def norm(basis_gram, projected, mean, square):
        direction = moments(projected, mean[...], square[...])[2]
        turned = jnp.dot(
            basis_gram,
            direction,
            precision=lax.Precision.HIGHEST,
            preferred_element_type=jnp.float32,
        )
        lanes = jnp.sum(direction * turned, axis=0, keepdims=True)
        return jnp.sum(lanes, axis=1, keepdims=True)

    partial = (
        norm(gram_pair[:rank, :rank], proj[:, :width], qm, qs)
        + norm(gram_pair[rank:, rank:], proj[:, width : 2 * width], vm, vs)
        + norm(gram_output, proj[:, 2 * width :], om, os)
    )
    square_own[...] = jnp.broadcast_to(partial, square_own.shape)
    shares = []
    for k in range(1, tp):
        copy = pltpu.make_async_remote_copy(
            src_ref=square_own,
            dst_ref=square_in.at[k - 1],
            send_sem=tp_send.at[k - 1],
            recv_sem=tp_recv.at[k - 1],
            device_id={"tp": lax.rem(column + k, tp)},
            device_id_type=MESH,
        )
        copy.start()
        shares.append(copy)
    gathers[6].relay(2)
    gathers[5].relay(3)
    gathers[7].relay(2)
    gathers[6].relay(3)
    gathers[7].relay(3)
    for copy in shares:
        copy.wait_recv()
    whole_squares = square_own[...]
    for k in range(1, tp):
        whole_squares = whole_squares + square_in[k - 1]
    squares[...] = whole_squares
    for gather in gathers[2:]:
        gather.finish()
    for copy in sums + alls + shares:
        copy.wait_send()
    for gather in gathers:
        gather.drain()
    for keep in keeps:
        keep.wait()


def exchange(fs, tp, mixer, cell, grads, pair, output_basis, weights, means, olds):
    share = pair.shape[1] // 2 // fs
    total = sum(grad.shape[1] for grad in grads)
    rank = means[0].shape[0]
    bf16, f32 = jnp.bfloat16, jnp.float32
    places = max(fs - 1, 16)
    hbm, vmem = pl.BlockSpec(memory_space=pl.ANY), pl.BlockSpec(memory_space=pltpu.VMEM)
    dma = pltpu.SemaphoreType.DMA

    def whole(array):
        return jax.ShapeDtypeStruct((array.shape[0] * fs, array.shape[1]), bf16)

    return pl.pallas_call(
        functools.partial(kernel, fs, tp),
        out_shape=(
            *(whole(weight) for weight in weights),
            whole(pair),
            whole(output_basis),
            jax.ShapeDtypeStruct((rank, total), f32),
            jax.ShapeDtypeStruct((8, 128), f32),
        ),
        in_specs=[hbm] * 10 + [vmem] * 6,
        out_specs=(hbm,) * 3 + (vmem,) * 4,
        scratch_shapes=[
            *(pltpu.VMEM(array.shape, bf16) for array in (mixer, cell, *grads, *weights)),
            pltpu.VMEM((rank, total), f32),
            pltpu.VMEM((fs - 1, share, total), f32),
            pltpu.VMEM((8, 128), f32),
            pltpu.VMEM((tp - 1, 8, 128), f32),
            dma((8, places)),
            dma((8, places)),
            dma((fs - 1,)),
            dma((fs - 1,)),
            dma((fs - 1,)),
            dma((fs - 1,)),
            dma((tp - 1,)),
            dma((tp - 1,)),
            dma((13,)),
        ],
        compiler_params=pltpu.CompilerParams(
            collective_id=0, has_side_effects=True, vmem_limit_bytes=50 * 1024 * 1024
        ),
    )(mixer, cell, *grads, pair, output_basis, *weights, *means, *olds)


def body(fs, tp):
    def local(
        mixer_input,
        cell_output,
        query_grad,
        value_grad,
        output_grad,
        query_weight,
        value_weight,
        output_weight,
        query_basis,
        value_basis,
        output_basis,
        query_mean,
        value_mean,
        output_mean,
        query_square,
        value_square,
        output_square,
    ):
        rank = query_basis.shape[1]
        means = (query_mean, value_mean, output_mean)
        olds = (query_square, value_square, output_square)
        *weights, whole_pair, whole_output, projected, squares = exchange(
            fs,
            tp,
            mixer_input,
            cell_output,
            (query_grad, value_grad, output_grad),
            jnp.concatenate([query_basis, value_basis], axis=1),
            output_basis,
            [w.astype(jnp.bfloat16) for w in (query_weight, value_weight, output_weight)],
            means,
            olds,
        )
        width = query_grad.shape[1]
        proj = (
            projected[:, :width],
            projected[:, width : 2 * width],
            projected[:, 2 * width :],
        )
        firsts, seconds, dirs = zip(*(moments(*each) for each in zip(proj, means, olds)))
        bases = (whole_pair[:, :rank], whole_pair[:, rank:], whole_output)
        factor = 1.0 / jnp.sqrt(squares[0, 0] / (3.0 * MODEL * CELL) + floor_mean)
        pairs = [jnp.concatenate(split(d), axis=0) for d in dirs]
        steps = [
            -factor * matmul(twice(b), d)
            for b, d in zip((query_basis, value_basis, output_basis), pairs)
        ]
        copies = [
            (w.astype(jnp.float32) + (-learn_rate * factor) * matmul(twice(b), d)).astype(
                jnp.bfloat16
            )
            for w, b, d in zip(weights, bases, pairs)
        ]
        return (*steps, *copies, *firsts, *seconds)

    return local


def solution(mesh):
    rows, split_both, columns = P("fs", None), P("fs", "tp"), P(None, "tp")
    in_specs = (rows,) * 2 + (split_both,) * 6 + (rows,) * 3 + (columns,) * 6
    out_specs = (split_both,) * 3 + (columns,) * 9
    return jax.shard_map(
        body(mesh.shape["fs"], mesh.shape["tp"]),
        mesh=mesh,
        in_specs=in_specs,
        out_specs=out_specs,
        check_vma=False,
    )
```

```python
import functools

import jax
import jax.numpy as jnp
from jax import lax
from jax.experimental import pallas as pl
from jax.experimental.pallas import tpu as pltpu
from jax.sharding import PartitionSpec as P

MODEL = 4096
CELL = 2048


beta_first = 0.8
beta_second = 0.9
floor_mean = 0.005
learn_rate = 0.05

MESH = pl.DeviceIdType.MESH


def matmul(left, right):
    return jnp.dot(left, right, preferred_element_type=jnp.float32)


def split(value):
    high = lax.reduce_precision(value, 8, 7)
    return high.astype(jnp.bfloat16), (value - high).astype(jnp.bfloat16)


def moments(projected, mean_old, square_old):
    moment_one = beta_first * mean_old + (1.0 - beta_first) * projected
    moment_two = beta_second * square_old + (1.0 - beta_second) * projected * projected
    return (moment_one, moment_two, moment_one / jnp.sqrt(moment_two))


def twice(basis):
    return jnp.concatenate([basis, basis], axis=1)


class Gather:
    def __init__(self, number, own, whole, block, half, me, count, by_line, send_sem, recv_sem):
        self.number, self.whole, self.block, self.half = number, whole, block, half
        self.me, self.count, self.by_line = me, count, by_line
        self.send_sem, self.recv_sem = send_sem, recv_sem
        self.rows = block // 2 if half is not None else block
        self.sent = []
        self.relayed = count == 8
        self.place, self.side = me // 2, lax.rem(me, 2)
        self.own = self.slot(me) if own is None else own

    def index(self, step, other=False):
        place = lax.rem(self.place + step + 4, 4)
        return place * 2 + (1 - self.side if other else self.side)

    def slot(self, origin):
        start = pl.multiple_of(origin * self.block, self.block)
        if self.half:
            start = pl.multiple_of(start + self.rows, self.rows)
        return self.whole.at[pl.ds(start, self.rows), :]

    def send(self, role, origin, target, inside=None, source=None):
        copy = pltpu.make_async_remote_copy(
            src_ref=self.slot(origin) if source is None else source,
            dst_ref=self.slot(origin),
            send_sem=self.send_sem.at[self.number, len(self.sent)],
            recv_sem=self.recv_sem.at[self.number, role],
            device_id={"fs": target},
            device_id_type=MESH,
        )
        self.sent.append((copy, inside))
        if inside is None:
            copy.start()
        else:
            pl.when(inside)(copy.start)

    def arrive(self, role, origin, inside=None):
        copy = pltpu.make_async_remote_copy(
            src_ref=self.slot(origin),
            dst_ref=self.slot(origin),
            send_sem=self.send_sem.at[self.number, 0],
            recv_sem=self.recv_sem.at[self.number, role],
            device_id={"fs": lax.rem(self.me + 1, self.count)},
            device_id_type=MESH,
        )
        if inside is None:
            copy.wait_recv()
        else:
            pl.when(inside)(copy.wait_recv)

    def start(self):
        if self.relayed:
            self.send(0, self.me, self.index(1), self.place < 3, self.own)
            self.send(3, self.me, self.index(-1), self.place > 0, self.own)
            self.send(6, self.me, self.index(0, True), None, self.own)
        else:
            for k in range(1, self.count):
                self.send(k - 1, self.me, lax.rem(self.me + k, self.count), None, self.own)

    def relay(self, distance):
        if not self.relayed:
            return
        place = self.place
        across = not (self.by_line and distance == 1)
        cross = self.index(0, True)
        if not across:
            self.arrive(6, cross)
            self.send(7, cross, self.index(1), place < 3)
            self.send(10, cross, self.index(-1), place > 0)
        below, above = self.index(-distance), self.index(distance)
        from_below, from_above = place >= distance, place + distance < 4
        self.arrive(distance - 1, below, from_below)
        if distance < 3:
            self.send(distance, below, self.index(1), (place >= distance) & (place < 3))
        if across:
            self.send(6 + distance, below, cross, from_below)
        self.arrive(2 + distance, above, from_above)
        if distance < 3:
            self.send(3 + distance, above, self.index(-1), from_above & (place > 0))
        if across:
            self.send(9 + distance, above, cross, from_above)

    def finish(self):
        if not self.relayed:
            for k in range(1, self.count):
                self.arrive(k - 1, lax.rem(self.me + self.count - k, self.count))
            return
        if not self.by_line:
            self.arrive(6, self.index(0, True))
        for distance in range(1, 4):
            self.arrive(6 + distance, self.index(-distance, True), self.place >= distance)
            self.arrive(9 + distance, self.index(distance, True), self.place + distance < 4)

    def drain(self):
        for copy, inside in self.sent:
            if inside is None:
                copy.wait_send()
            else:
                pl.when(inside)(copy.wait_send)


def kernel(
    fs,
    tp,
    mixer_hbm,
    cell_hbm,
    qg_hbm,
    vg_hbm,
    og_hbm,
    pair_hbm,
    ob_hbm,
    qw_hbm,
    vw_hbm,
    ow_hbm,
    qm,
    vm,
    om,
    qs,
    vs,
    os,
    qw_all,
    vw_all,
    ow_all,
    pair_all,
    ob_all,
    proj,
    squares,
    mixer,
    cell,
    qg,
    vg,
    og,
    qw,
    vw,
    ow,
    part,
    parts,
    square_own,
    square_in,
    send_sem,
    recv_sem,
    sum_send,
    sum_recv,
    tp_send,
    tp_recv,
    local_sem,
):
    me, column = lax.axis_index("fs"), lax.axis_index("tp")
    rank, width = qm.shape
    gathers = [
        Gather(0, None, pair_all, pair_hbm.shape[0], None, me, fs, False, send_sem, recv_sem),
        Gather(1, None, ob_all, ob_hbm.shape[0], None, me, fs, True, send_sem, recv_sem),
    ]
    kept = ((qw, qw_all), (vw, vw_all), (ow, ow_all))
    for own, whole in kept:
        block = own.shape[0]
        for half in range(2):
            piece = own.at[pl.ds(half * (block // 2), block // 2), :]
            gathers.append(
                Gather(
                    len(gathers), piece, whole, block, half, me, fs, half == 0, send_sem, recv_sem
                )
            )
    loads = [
        pltpu.make_async_copy(source, target, local_sem.at[i])
        for i, (source, target) in enumerate(
            (
                (pair_hbm, gathers[0].own),
                (ob_hbm, gathers[1].own),
                (qw_hbm, qw),
                (vw_hbm, vw),
                (ow_hbm, ow),
                (cell_hbm, cell),
                (og_hbm, og),
                (mixer_hbm, mixer),
                (qg_hbm, qg),
                (vg_hbm, vg),
            )
        )
    ]
    for load in loads:
        load.start()

    barrier = pltpu.get_barrier_semaphore()
    for k in range(1, fs):
        pl.semaphore_signal(
            barrier, inc=1, device_id={"fs": lax.rem(me + k, fs)}, device_id_type=MESH
        )
    for k in range(1, tp):
        pl.semaphore_signal(
            barrier, inc=1, device_id={"tp": lax.rem(column + k, tp)}, device_id_type=MESH
        )
    pl.semaphore_wait(barrier, fs + tp - 2)

    loads[0].wait()
    gathers[0].start()
    loads[1].wait()
    gathers[1].start()
    loads[2].wait()
    gathers[2].start()
    for distance in range(1, 4):
        gathers[0].relay(distance)
        gathers[1].relay(distance)
    gathers[3].start()
    loads[3].wait()
    gathers[4].start()
    gathers[5].start()
    loads[4].wait()
    gathers[6].start()
    gathers[7].start()
    keeps = []
    for i, (own, whole) in enumerate(kept):
        rows = own.shape[0]
        place = whole.at[pl.ds(pl.multiple_of(me * rows, rows), rows), :]
        keeps.append(pltpu.make_async_copy(own, place, local_sem.at[10 + i]))
    for keep in keeps:
        keep.start()
    gathers[2].relay(1)
    for load in loads[5:]:
        load.wait()
    part[...] = jnp.zeros_like(part)
    gathers[0].finish()
    gathers[1].finish()

    tile = 256

    def project(rows, grad):
        turned = jnp.transpose(rows)
        high = turned.astype(jnp.bfloat16)
        low = (turned - high.astype(jnp.float32)).astype(jnp.bfloat16)
        both = matmul(jnp.concatenate([high, low], axis=0), grad)
        return both[:rank] + both[rank:]

    def step(t, carry):
        at = pl.ds(pl.multiple_of(t * tile, tile), tile)
        rows = matmul(mixer[at, :], pair_all[...])
        part[:, :width] += project(rows[:, :rank], qg[at, :])
        part[:, width : 2 * width] += project(rows[:, rank:], vg[at, :])
        part[:, 2 * width :] += project(matmul(cell[at, :], ob_all[...]), og[at, :])
        return carry

    lax.fori_loop(0, mixer.shape[0] // tile, step, 0)

    share = rank // fs

    def strip(index):
        return pl.ds(pl.multiple_of(index * share, share), share)

    sums = []
    for k in range(1, fs):
        target = lax.rem(me + k, fs)
        copy = pltpu.make_async_remote_copy(
            src_ref=part.at[strip(target), :],
            dst_ref=parts.at[k - 1],
            send_sem=sum_send.at[k - 1],
            recv_sem=sum_recv.at[k - 1],
            device_id={"fs": target},
            device_id_type=MESH,
        )
        copy.start()
        sums.append(copy)
    gathers[3].relay(1)
    gathers[2].relay(2)
    gathers[4].relay(1)
    gathers[3].relay(2)
    gathers[2].relay(3)

    def gram(whole, block):
        def add(i, total):
            piece = whole[pl.ds(pl.multiple_of(i * block, block), block), :]
            turned = jnp.transpose(piece.astype(jnp.float32)).astype(jnp.bfloat16)
            return total + matmul(turned, piece)

        size = whole.shape[1]
        return lax.fori_loop(
            0, whole.shape[0] // block, add, jnp.zeros((size, size), jnp.float32)
        )

    for copy in sums:
        copy.wait_recv()
    total = part[strip(me), :]
    for k in range(1, fs):
        total = total + parts[k - 1]
    proj[strip(me), :] = total
    gram_pair = gram(pair_all, 256)
    gram_output = gram(ob_all, 256)
    strips = Gather(8, None, proj, share, None, me, fs, False, send_sem, recv_sem)
    strips.start()
    gathers[5].relay(1)
    strips.relay(1)
    gathers[4].relay(2)
    gathers[3].relay(3)
    strips.relay(2)
    gathers[6].relay(1)
    gathers[5].relay(2)
    strips.relay(3)
    gathers[4].relay(3)
    gathers[7].relay(1)
    strips.finish()

    def norm(basis_gram, projected, mean, square):
        direction = moments(projected, mean[...], square[...])[2]
        turned = jnp.dot(
            basis_gram,
            direction,
            precision=lax.Precision.HIGHEST,
            preferred_element_type=jnp.float32,
        )
        lanes = jnp.sum(direction * turned, axis=0, keepdims=True)
        return jnp.sum(lanes, axis=1, keepdims=True)

    partial = (
        norm(gram_pair[:rank, :rank], proj[:, :width], qm, qs)
        + norm(gram_pair[rank:, rank:], proj[:, width : 2 * width], vm, vs)
        + norm(gram_output, proj[:, 2 * width :], om, os)
    )
    square_own[...] = jnp.broadcast_to(partial, square_own.shape)
    shares = []
    for k in range(1, tp):
        copy = pltpu.make_async_remote_copy(
            src_ref=square_own,
            dst_ref=square_in.at[k - 1],
            send_sem=tp_send.at[k - 1],
            recv_sem=tp_recv.at[k - 1],
            device_id={"tp": lax.rem(column + k, tp)},
            device_id_type=MESH,
        )
        copy.start()
        shares.append(copy)
    gathers[6].relay(2)
    gathers[5].relay(3)
    gathers[7].relay(2)
    gathers[6].relay(3)
    gathers[7].relay(3)
    for copy in shares:
        copy.wait_recv()
    whole_squares = square_own[...]
    for k in range(1, tp):
        whole_squares = whole_squares + square_in[k - 1]
    squares[...] = whole_squares
    for gather in gathers[2:]:
        gather.finish()
    for copy in sums + shares:
        copy.wait_send()
    for gather in gathers + [strips]:
        gather.drain()
    for keep in keeps:
        keep.wait()


def exchange(fs, tp, mixer, cell, grads, pair, output_basis, weights, means, olds):
    share = pair.shape[1] // 2 // fs
    total = sum(grad.shape[1] for grad in grads)
    rank = means[0].shape[0]
    bf16, f32 = jnp.bfloat16, jnp.float32
    places = max(fs - 1, 16)
    hbm, vmem = pl.BlockSpec(memory_space=pl.ANY), pl.BlockSpec(memory_space=pltpu.VMEM)
    dma = pltpu.SemaphoreType.DMA

    def whole(array):
        return jax.ShapeDtypeStruct((array.shape[0] * fs, array.shape[1]), bf16)

    return pl.pallas_call(
        functools.partial(kernel, fs, tp),
        out_shape=(
            *(whole(weight) for weight in weights),
            whole(pair),
            whole(output_basis),
            jax.ShapeDtypeStruct((rank, total), f32),
            jax.ShapeDtypeStruct((8, 128), f32),
        ),
        in_specs=[hbm] * 10 + [vmem] * 6,
        out_specs=(hbm,) * 3 + (vmem,) * 4,
        scratch_shapes=[
            *(pltpu.VMEM(array.shape, bf16) for array in (mixer, cell, *grads, *weights)),
            pltpu.VMEM((rank, total), f32),
            pltpu.VMEM((fs - 1, share, total), f32),
            pltpu.VMEM((8, 128), f32),
            pltpu.VMEM((tp - 1, 8, 128), f32),
            dma((9, places)),
            dma((9, places)),
            dma((fs - 1,)),
            dma((fs - 1,)),
            dma((tp - 1,)),
            dma((tp - 1,)),
            dma((13,)),
        ],
        compiler_params=pltpu.CompilerParams(
            collective_id=0, has_side_effects=True, vmem_limit_bytes=50 * 1024 * 1024
        ),
    )(mixer, cell, *grads, pair, output_basis, *weights, *means, *olds)


def body(fs, tp):
    def local(
        mixer_input,
        cell_output,
        query_grad,
        value_grad,
        output_grad,
        query_weight,
        value_weight,
        output_weight,
        query_basis,
        value_basis,
        output_basis,
        query_mean,
        value_mean,
        output_mean,
        query_square,
        value_square,
        output_square,
    ):
        rank = query_basis.shape[1]
        means = (query_mean, value_mean, output_mean)
        olds = (query_square, value_square, output_square)
        *weights, whole_pair, whole_output, projected, squares = exchange(
            fs,
            tp,
            mixer_input,
            cell_output,
            (query_grad, value_grad, output_grad),
            jnp.concatenate([query_basis, value_basis], axis=1),
            output_basis,
            [w.astype(jnp.bfloat16) for w in (query_weight, value_weight, output_weight)],
            means,
            olds,
        )
        width = query_grad.shape[1]
        proj = (
            projected[:, :width],
            projected[:, width : 2 * width],
            projected[:, 2 * width :],
        )
        firsts, seconds, dirs = zip(*(moments(*each) for each in zip(proj, means, olds)))
        bases = (whole_pair[:, :rank], whole_pair[:, rank:], whole_output)
        factor = 1.0 / jnp.sqrt(squares[0, 0] / (3.0 * MODEL * CELL) + floor_mean)
        pairs = [jnp.concatenate(split(d), axis=0) for d in dirs]
        steps = [
            -factor * matmul(twice(b), d)
            for b, d in zip((query_basis, value_basis, output_basis), pairs)
        ]
        copies = [
            (w.astype(jnp.float32) + (-learn_rate * factor) * matmul(twice(b), d)).astype(
                jnp.bfloat16
            )
            for w, b, d in zip(weights, bases, pairs)
        ]
        return (*steps, *copies, *firsts, *seconds)

    return local


def solution(mesh):
    rows, split_both, columns = P("fs", None), P("fs", "tp"), P(None, "tp")
    in_specs = (rows,) * 2 + (split_both,) * 6 + (rows,) * 3 + (columns,) * 6
    out_specs = (split_both,) * 3 + (columns,) * 9
    return jax.shard_map(
        body(mesh.shape["fs"], mesh.shape["tp"]),
        mesh=mesh,
        in_specs=in_specs,
        out_specs=out_specs,
        check_vma=False,
    )
```
